32 devices in a mesh: rep: 2 (over y), fs: 4 (over z), tp: 4 (over x, core).
Axes of the slice: x: 2, y: 2, z: 4, core: 2. Of those that a mesh axis runs over, the one named last changes fastest.
Arguments:
- stream: bfloat16 [4096, 2048], P(('rep', 'fs', 'tp')), may hold values from -6 to 6
- gain_before: float32 [2048], replicated, may hold values from 0.1 to 1.9
- gain_after: float32 [2048], replicated, may hold values from 0.1 to 1.9
- proj_gate: bfloat16 [2048, 3584], P('fs', 'tp'), may hold values from -0.125 to 0.125
- proj_lift: bfloat16 [2048, 3584], P('fs', 'tp'), may hold values from -0.125 to 0.125
- proj_down: bfloat16 [3584, 2048], P('tp', 'fs'), may hold values from -0.09375 to 0.09375
- mixer_gain: float32 [2048], replicated, may hold values from 0.1 to 1.9
- mixer_u: bfloat16 [2048, 2048], P('fs', 'tp'), may hold values from -0.125 to 0.125
- mixer_v: bfloat16 [2048, 2048], P('fs', 'tp'), may hold values from -1 to 1
- layer_gain: float32 [2048], P('tp'), may hold values from 0.1 to 1.9
- layer_shift: float32 [2048], P('tp'), may hold values from -3 to 3
- spatial: bfloat16 [16, 128, 128], P('tp'), may hold values from -0.5 to 0.5
- spatial_shift: float32 [16, 128], P('tp'), may hold values from 0.2 to 2
- mixer_down: bfloat16 [2048, 2048], P('tp', 'fs'), may hold values from -0.125 to 0.125
Outputs:
- result: bfloat16 [4096, 2048], P(('rep', 'fs', 'tp'))
The draws below stay inside these ranges and needn't reach their ends.
All inputs are finite; a program needn't handle non-finite values.
Results may differ from the reference program's by a relative error of at most 0.017.
Values may be sent and summed in bfloat16 or wider, within the bound.
No kernel may reach another device: no remote copies, remote signals or barrier semaphores. Data moves between devices by JAX's collectives and lax.ppermute only.
A program may use at most 128 MiB of HBM per device.

```python
import jax
import jax.numpy as jnp
from jax import lax

D = 2048
FF = 3584
GROUPS = 16
GROUP_DIM = 128
SPAN = 128
TOK = 512
A = 2048
TOKENS = 4096
N_TP = 4


def draw_mixer_v(key, part):
    first_key, second_key = jax.random.split(key)
    position = jnp.arange(A, dtype=jnp.float32) / (A - 1)
    rising = 4.0
    basis = jnp.clip(jax.random.normal(first_key, (D, A), jnp.float32), -4.0, 4.0)
    jitter = jnp.exp(jax.random.uniform(second_key, (A,), jnp.float32, -0.3, 0.3))
    column_scale = rising ** (position - 0.5) * jitter
    return jnp.clip(basis * column_scale * D ** (-0.5), -1.0, 1.0).astype(jnp.bfloat16)


def levels(own_key, dims, pieces, low, high):
    def one(dim, blocks):
        draws = jax.random.uniform(jax.random.fold_in(jax.random.fold_in(own_key, 6), dim), (blocks,), jnp.float32, low / len(pieces), high / len(pieces))
        return jnp.repeat(jnp.exp(draws), dims[dim] // blocks).reshape((-1,) + (1,) * (len(dims) - dim - 1))

    factor_of = one(*pieces[0])
    for cut in pieces[1:]:
        factor_of = factor_of * one(*cut)
    return factor_of


def noise(rng, extent, scale, reach, shards=(), kind=jnp.bfloat16):
    result = scale * jax.random.normal(rng, extent, jnp.float32)
    if shards:
        result = result * levels(rng, extent, shards, -0.22, 0.18)
    return jnp.clip(result, -reach, reach).astype(kind)


def setup_inputs(seed: int = 0) -> dict:
    keys = jax.random.split(jax.random.key(seed), 15)
    stream = noise(keys[0], (TOKENS, D), 1.0, 6.0, ((0, 32),))
    gain_before = jnp.clip(1.0 + 0.18 * jax.random.normal(keys[1], (D,), jnp.float32), 0.1, 1.9)
    gain_after = jnp.clip(1.0 + 0.18 * jax.random.normal(keys[2], (D,), jnp.float32), 0.1, 1.9)
    proj_gate = noise(keys[3], (D, FF), D ** -0.5, 0.125, ((0, 4), (1, 4)))
    proj_lift = noise(keys[4], (D, FF), D ** -0.5, 0.125, ((0, 4), (1, 4)))
    proj_down = noise(keys[5], (FF, D), FF ** -0.5, 0.09375, ((0, 4), (1, 4)))
    mixer_gain = jnp.clip(1.0 + 0.18 * jax.random.normal(keys[6], (D,), jnp.float32), 0.1, 1.9)
    mixer_u = noise(keys[7], (D, A), D ** -0.5, 0.125, ((0, 4), (1, 4)))
    mixer_v = draw_mixer_v(jax.random.fold_in(keys[14], 71), 0)
    layer_gain = jnp.clip(1.0 + 0.18 * jax.random.normal(keys[9], (A,), jnp.float32), 0.1, 1.9)
    layer_shift = noise(keys[10], (A,), 0.5, 3.0, ((0, 4),), jnp.float32)
    spatial = noise(keys[11], (GROUPS, SPAN, SPAN), SPAN ** -0.5, 0.5, ((0, 4),))
    spatial_shift = jnp.clip(0.2 + 1.8 * jax.random.uniform(keys[12], (GROUPS, SPAN), jnp.float32) ** levels(keys[12], (GROUPS, SPAN), ((0, 4),), -0.2, 0.2), 0.2, 2.0)
    mixer_down = noise(keys[13], (A, D), A ** -0.5, 0.125, ((0, 4), (1, 4)))
    return {"stream": stream, "gain_before": gain_before, "gain_after": gain_after, "proj_gate": proj_gate, "proj_lift": proj_lift, "proj_down": proj_down, "mixer_gain": mixer_gain, "mixer_u": mixer_u, "mixer_v": mixer_v, "layer_gain": layer_gain, "layer_shift": layer_shift, "spatial": spatial, "spatial_shift": spatial_shift, "mixer_down": mixer_down}


norm_epsilon = 1e-06
layer_epsilon = 1e-05

def norm_rows(row_block, scale_gain):
    widened = row_block.astype(jnp.float32)
    factor = lax.rsqrt(lax.optimization_barrier(jnp.mean(widened * widened, axis=1, keepdims=True)) + norm_epsilon)
    return (widened * factor * scale_gain).astype(jnp.bfloat16)

def blocked_sum(left_rows, right_rows):
    unit_count = left_rows.shape[1] // N_TP
    running = jnp.zeros((left_rows.shape[0], right_rows.shape[1]), jnp.float32)
    for member in range(N_TP):
        partial_value = jnp.dot(left_rows[:, member * unit_count:(member + 1) * unit_count], right_rows[member * unit_count:(member + 1) * unit_count], preferred_element_type=jnp.float32)
        running = running + lax.optimization_barrier(partial_value.astype(jnp.bfloat16)).astype(jnp.float32)
    return running

def half_step(row_block, scale_gain, proj_gate, proj_lift, proj_down):
    normed = norm_rows(row_block, scale_gain)
    gate_vals = jnp.dot(normed, proj_gate, preferred_element_type=jnp.float32)
    lift_vals = jnp.dot(normed, proj_lift, preferred_element_type=jnp.float32)
    hidden = (jax.nn.silu(gate_vals) * lift_vals).astype(jnp.bfloat16)
    delta = blocked_sum(hidden, proj_down)
    return (row_block.astype(jnp.float32) + 0.5 * delta).astype(jnp.bfloat16)

def token_mixer(row_block, mixer_gain, mixer_u, mixer_v, layer_gain, layer_shift, spatial, spatial_shift, mixer_down):
    normed = norm_rows(row_block, mixer_gain)
    u_vals = jnp.dot(normed, mixer_u, preferred_element_type=jnp.float32)
    v_vals = jnp.dot(normed, mixer_v, preferred_element_type=jnp.float32)
    lifted = jax.nn.gelu(v_vals)
    centre = lax.optimization_barrier(jnp.mean(lifted, axis=1, keepdims=True))
    spread = lax.optimization_barrier(jnp.mean(jnp.square(lifted - centre), axis=1, keepdims=True))
    normed_v = ((lifted - centre) * lax.rsqrt(spread + layer_epsilon) * layer_gain + layer_shift).astype(jnp.bfloat16)
    blocked = normed_v.reshape(TOK // SPAN, SPAN, GROUPS, GROUP_DIM).astype(jnp.float32)
    causal = jnp.tril(jnp.ones((SPAN, SPAN), dtype=bool))
    masked = jnp.where(causal[None], spatial.astype(jnp.float32), jnp.float32(0.0))
    mixed_v = jnp.einsum('gts,bsgd->btgd', masked, blocked) + spatial_shift.T[None, :, :, None]
    gated = (jax.nn.gelu(u_vals) * mixed_v.reshape(TOK, GROUPS * GROUP_DIM)).astype(jnp.bfloat16)
    delta = blocked_sum(gated, mixer_down)
    return (row_block.astype(jnp.float32) + delta).astype(jnp.bfloat16)

def reference(stream, gain_before, gain_after, proj_gate, proj_lift, proj_down, mixer_gain, mixer_u, mixer_v, layer_gain, layer_shift, spatial, spatial_shift, mixer_down):

    def one_sequence(row_block):
        first = half_step(row_block, gain_before, proj_gate, proj_lift, proj_down)
        second = token_mixer(first, mixer_gain, mixer_u, mixer_v, layer_gain, layer_shift, spatial, spatial_shift, mixer_down)
        return half_step(second, gain_after, proj_gate, proj_lift, proj_down)
    stacked = stream.reshape(stream.shape[0] // TOK, TOK, stream.shape[1])
    return lax.map(one_sequence, stacked).reshape(stream.shape)
```

```python
import jax
import jax.numpy as jnp
from jax import lax
from jax.sharding import PartitionSpec as P

GROUP_DIM = 128
SPAN = 128
CORES = 2

norm_epsilon = 1e-06
layer_epsilon = 1e-05


def rotation(count, shift):
    return [(i, (i + shift) % count) for i in range(count)]


class Layout:
    def __init__(self, sizes):
        self.reps = sizes["rep"]
        self.shards = sizes["fs"]
        self.chips = sizes["tp"] // CORES
        self.rep = lax.axis_index("rep")
        self.fs = lax.axis_index("fs")

    def shift_fs(self, value, shift):
        return lax.ppermute(value, "fs", rotation(self.shards, shift))

    def shift_rep(self, value, shift):
        return lax.ppermute(value, "rep", rotation(self.reps, shift))

    def shift_chip(self, value, shift):
        pairs = [
            (chip * CORES + core, ((chip + shift) % self.chips) * CORES + core)
            for chip in range(self.chips)
            for core in range(CORES)
        ]
        return lax.ppermute(value, "tp", pairs)

    def swap_core(self, value):
        pairs = [
            (chip * CORES + core, chip * CORES + 1 - core)
            for chip in range(self.chips)
            for core in range(CORES)
        ]
        return lax.ppermute(value, "tp", pairs)

    def slot_order(self):
        ahead = (self.shards) // 2
        return list(range(1, ahead + 1)), list(range(self.shards - 1, ahead, -1))

    def blocks(self):
        order = [self.fs * self.reps + j for j in range(self.reps)]
        ahead, behind = self.slot_order()
        for slot in ahead + behind:
            shard = (self.fs - slot) % self.shards
            for j in range(self.reps):
                order.append(shard * self.reps + (self.rep - j) % self.reps)
        return order

    def to_own(self, value):
        width = value.shape[-1] // (self.shards * self.reps)
        parts = [
            lax.dynamic_slice_in_dim(value, index * width, width, axis=value.ndim - 1)
            for index in self.blocks()
        ]
        return jnp.concatenate(parts, axis=-1)

    def from_own(self, value):
        width = value.shape[-1] // (self.shards * self.reps)
        out = jnp.zeros_like(value)
        for place, index in enumerate(self.blocks()):
            part = value[:, place * width : (place + 1) * width]
            out = lax.dynamic_update_slice_in_dim(out, part, index * width, axis=1)
        return out

    def gather_weight(self, shard, axis):
        width = shard.shape[axis] // self.reps
        piece = lax.dynamic_slice_in_dim(shard, self.rep * width, width, axis=axis)
        ahead, behind = self.slot_order()
        pieces = {}
        for slots, shift in ((ahead, 1), (behind, -1)):
            moving = piece
            for slot in slots:
                moving = self.shift_fs(moving, shift)
                pieces[slot] = [moving]
        for slot in ahead + behind:
            for j in range(1, self.reps):
                pieces[slot].append(self.shift_rep(pieces[slot][0], j))
        out = [shard]
        for slot in ahead + behind:
            out.extend(pieces[slot])
        return out

    def gather_rows(self, rows):
        out = [rows, self.swap_core(rows)]
        for j in range(1, self.chips):
            far = self.shift_chip(rows, j)
            out.extend([far, self.swap_core(far)])
        return jnp.concatenate(out, axis=0)

    def scatter_rows(self, partial_value, count):
        wide = jnp.float32
        blocks = [
            partial_value[i * count : (i + 1) * count] for i in range(CORES * self.chips)
        ]
        total = None
        for j in range(self.chips - 1, -1, -1):
            mine = blocks[CORES * j].astype(wide)
            summed = mine + self.swap_core(blocks[CORES * j + 1]).astype(wide)
            if j:
                summed = self.shift_chip(summed.astype(jnp.bfloat16), -j).astype(wide)
            total = summed if total is None else total + summed
        return total

    def sum_stats(self, stats, count):
        shape = (self.chips, CORES, count, stats.shape[1])
        own = stats.reshape(shape)
        pair = own + self.swap_core(own)[:, ::-1]
        total = pair
        for j in range(1, self.chips):
            total = total + jnp.roll(self.shift_chip(pair, j), j, axis=0)
        return total.reshape(stats.shape)


def norm_rows(row_block, scale_gain):
    widened = row_block.astype(jnp.float32)
    factor = lax.rsqrt(jnp.mean(widened * widened, axis=1, keepdims=True) + norm_epsilon)
    return (widened * factor * scale_gain).astype(jnp.bfloat16)


def dot(left, right):
    return jnp.dot(left, right, preferred_element_type=jnp.float32)


def half_again(place, rows, scale_gain, gate, lift, down):
    count = rows.shape[0]
    normed = place.gather_rows(norm_rows(rows, scale_gain))
    gate_vals = dot(normed, gate)
    lift_vals = dot(normed, lift)
    hidden = (jax.nn.silu(gate_vals) * lift_vals).astype(jnp.bfloat16)
    partial_value = dot(hidden, down).astype(jnp.bfloat16)
    summed = place.scatter_rows(partial_value, count)
    return (rows.astype(jnp.float32) + 0.5 * summed).astype(jnp.bfloat16)


def token_mixer(
    place, rows, mixer_gain, u_mat, v_mat, layer_gain, layer_shift, spatial, spatial_shift, down
):
    count = rows.shape[0]
    normed = place.gather_rows(norm_rows(rows, mixer_gain))
    tokens = normed.shape[0]
    channels = layer_gain.shape[0] * CORES * place.chips
    lifted = jax.nn.gelu(dot(normed, v_mat))
    stats = jnp.stack([jnp.sum(lifted, axis=1), jnp.sum(lifted * lifted, axis=1)], axis=1)
    stats = place.sum_stats(stats, count)
    centre = stats[:, :1] / channels
    spread = stats[:, 1:] / channels - centre * centre
    normed_v = (
        (lifted - centre) * lax.rsqrt(spread + layer_epsilon) * layer_gain + layer_shift
    ).astype(jnp.bfloat16)
    groups_here = spatial.shape[0]
    blocked = normed_v.reshape(tokens // SPAN, SPAN, groups_here, GROUP_DIM)
    causal = jnp.tril(jnp.ones((SPAN, SPAN), dtype=bool))
    masked = jnp.where(causal[None], spatial, jnp.zeros((), jnp.bfloat16))
    mixed_v = jnp.einsum("gts,bsgd->btgd", masked, blocked, preferred_element_type=jnp.float32)
    mixed_v = mixed_v + spatial_shift.T[None, :, :, None]
    u_vals = dot(normed, u_mat)
    gated = (jax.nn.gelu(u_vals) * mixed_v.reshape(tokens, groups_here * GROUP_DIM)).astype(
        jnp.bfloat16
    )
    summed = place.scatter_rows(dot(gated, down).astype(jnp.bfloat16), count)
    return (rows.astype(jnp.float32) + summed).astype(jnp.bfloat16)


def make_body(sizes):
    def body(
        stream,
        gain_before,
        gain_after,
        proj_gate,
        proj_lift,
        proj_down,
        mixer_gain,
        mixer_u,
        mixer_v,
        layer_gain,
        layer_shift,
        spatial,
        spatial_shift,
        mixer_down,
    ):
        place = Layout(sizes)
        rows = place.to_own(stream)
        gain_before, gain_after, mixer_gain = (
            place.to_own(g) for g in (gain_before, gain_after, mixer_gain)
        )
        gate = jnp.concatenate(place.gather_weight(proj_gate, 0), axis=0)
        lift = jnp.concatenate(place.gather_weight(proj_lift, 0), axis=0)
        down = jnp.concatenate(place.gather_weight(proj_down, 1), axis=1)
        v_mat = jnp.concatenate(place.gather_weight(mixer_v, 0), axis=0)
        u_mat = jnp.concatenate(place.gather_weight(mixer_u, 0), axis=0)
        m_down = jnp.concatenate(place.gather_weight(mixer_down, 1), axis=1)
        first = half_again(place, rows, gain_before, gate, lift, down)
        second = token_mixer(
            place, first, mixer_gain, u_mat, v_mat, layer_gain, layer_shift, spatial,
            spatial_shift, m_down,
        )
        result = half_again(place, second, gain_after, gate, lift, down)
        return place.from_own(result)

    return body


def solution(mesh):
    sizes = dict(mesh.shape)
    placed = (
        P(("rep", "fs", "tp"), None),
        P(),
        P(),
        P("fs", "tp"),
        P("fs", "tp"),
        P("tp", "fs"),
        P(),
        P("fs", "tp"),
        P("fs", "tp"),
        P("tp"),
        P("tp"),
        P("tp", None, None),
        P("tp", None),
        P("tp", "fs"),
    )
    return jax.shard_map(
        make_body(sizes),
        mesh=mesh,
        in_specs=placed,
        out_specs=P(("rep", "fs", "tp"), None),
        check_vma=False,
    )
```

```python
import functools

import jax
import jax.numpy as jnp
from jax import lax
from jax.experimental import pallas as pl
from jax.experimental.pallas import tpu as pltpu
from jax.sharding import PartitionSpec as P


GROUP_DIM = 128
SPAN = 128
CORES = 2
LANES = 128
SUBLANES = 8
TILE = 256
HALVES = 2

norm_epsilon = 1e-06
layer_epsilon = 1e-05


ANY = pl.BlockSpec(memory_space=pl.ANY)
VMEM = pl.BlockSpec(memory_space=pltpu.VMEM)
SMEM = pl.BlockSpec(memory_space=pltpu.SMEM)
WIDE = jnp.float32
NARROW = jnp.bfloat16


def rotation(count, shift):
    return [(i, (i + shift) % count) for i in range(count)]


class Layout:
    def __init__(self, sizes):
        self.reps = sizes["rep"]
        self.shards = sizes["fs"]
        self.chips = sizes["tp"] // CORES
        self.members = sizes["tp"]
        self.rep = lax.axis_index("rep")
        self.fs = lax.axis_index("fs")

    def shift_fs(self, value, shift):
        return lax.ppermute(value, "fs", rotation(self.shards, shift))

    def shift_rep(self, value, shift):
        return lax.ppermute(value, "rep", rotation(self.reps, shift))

    def shift_tp(self, value, chip_shift, core_flip):
        pairs = [
            (
                chip * CORES + core,
                ((chip + chip_shift) % self.chips) * CORES + (core ^ core_flip),
            )
            for chip in range(self.chips)
            for core in range(CORES)
        ]
        return lax.ppermute(value, "tp", pairs)

    def parts(self, depth):
        return 1 if depth % (self.shards * self.reps * LANES) else self.reps

    def blocks(self, depth):
        reps = self.parts(depth)
        order = [self.fs * reps + j for j in range(reps)]
        for slot in range(1, self.shards):
            owner = (self.fs - slot + self.shards) % self.shards
            for j in range(reps):
                piece = (self.rep - j + self.reps) % self.reps if reps > 1 else 0
                order.append(owner * reps + piece)
        return order

    def order(self, depth):
        reps = self.parts(depth)
        slot = jnp.arange(self.shards, dtype=jnp.int32)[:, None]
        j = jnp.arange(reps, dtype=jnp.int32)[None]
        owner = (self.fs - slot + self.shards) % self.shards
        turned = (self.rep - j + self.reps) % self.reps if reps > 1 else j
        piece = jnp.where(slot == 0, j, turned)
        return (owner * reps + piece).reshape(-1).astype(jnp.int32)

    def from_own(self, value):
        order = self.blocks(value.shape[-1])
        width = value.shape[-1] // len(order)
        out = jnp.zeros_like(value)
        for i, index in enumerate(order):
            part = value[:, i * width : (i + 1) * width]
            out = lax.dynamic_update_slice_in_dim(out, part, index * width, axis=1)
        return out

    def gather_weight(self, shard, axis, direct=False):
        reps = self.parts(shard.shape[axis] * self.shards)
        width = shard.shape[axis] // reps
        first = self.rep * width if reps > 1 else 0
        piece = lax.dynamic_slice_in_dim(shard, first, width, axis=axis)
        moving, out = piece, [shard]
        for slot in range(1, self.shards):
            back = direct and slot == self.shards - 1
            moving = self.shift_fs(piece, -1) if back else self.shift_fs(moving, 1)
            out.append(moving)
            for j in range(1, reps):
                out.append(self.shift_rep(moving, j))
        return out

    def gather_rows(self, rows):
        near = self.shift_tp(rows, 0, 1)
        out = [rows, near]
        for j in range(1, self.chips):
            far = self.shift_tp(rows, j, 0)
            out.extend([far, self.shift_tp(far, 0, 1)])
        return out

    def pass_rows(self, rows):
        out = []
        for j in range(1, self.chips):
            far = self.shift_tp(rows, j, 0)
            out.extend([far, self.shift_tp(far, 0, 1)])
        return out

    def scatter_far(self, blocks):
        terms = []
        for j in range(self.chips - 1, 0, -1):
            near = self.shift_tp(blocks[CORES * j + 1], 0, 1)
            pair = (blocks[CORES * j].astype(WIDE) + near.astype(WIDE)).astype(NARROW)
            terms.append(self.shift_tp(pair, -j, 0))
        return terms

    def scatter_near(self, blocks):
        return [blocks[0], self.shift_tp(blocks[1], 0, 1)]

    def share_stats(self, stats):
        out = []
        for j in range(self.chips):
            for flip in range(CORES):
                same = j == 0 and flip == 0
                out.append(stats if same else self.shift_tp(stats, j, flip))
        return out


def dot(left, right):
    return jnp.dot(left, right, preferred_element_type=WIDE)


def column_tiles(width):
    if width % LANES or width <= TILE:
        return [(0, width)]
    starts = list(range(0, width - TILE + 1, TILE))
    ends = starts[1:] + [width]
    return [(a, b - a) for a, b in zip(starts, ends)]


def call(kernel, outs, scratch, flops, *args, specs, out_specs=None, room=24):
    return pl.pallas_call(
        kernel,
        out_shape=outs,
        in_specs=specs,
        out_specs=out_specs or [VMEM] * len(outs),
        scratch_shapes=scratch,
        compiler_params=pltpu.CompilerParams(vmem_limit_bytes=room * 2**20),
        cost_estimate=pl.CostEstimate(flops=flops, transcendentals=0, bytes_accessed=0),
    )(*args)


def shape(dims, kind):
    return jax.ShapeDtypeStruct(dims, kind)


def stack_copies(refs, target, sem, axis):
    out, start = [], 0
    for ref in refs:
        place = pl.ds(start, ref.shape[axis])
        start += ref.shape[axis]
        at = (place, slice(None)) if axis == 0 else (slice(None), place)
        out.append(pltpu.make_async_copy(ref, target.at[at], sem))
    return out


def begin(copies):
    for copy in copies:
        copy.start()


def finish(copies):
    for copy in copies:
        copy.wait()


def pack_kernel(axis, *refs):
    copies = stack_copies(refs[:-2], refs[-2], refs[-1], axis)
    begin(copies)
    finish(copies)


def pack_call(parts, axis):
    dims = list(parts[0].shape)
    dims[axis] = sum(part.shape[axis] for part in parts)
    return call(
        functools.partial(pack_kernel, axis),
        [shape(tuple(dims), NARROW)],
        [pltpu.SemaphoreType.DMA],
        1000000,
        *parts,
        specs=[ANY] * len(parts),
        out_specs=[ANY],
    )[0]


def hidden_kernel(blocks, *refs):
    rows = refs[:blocks]
    gate, lift, out, x_all, x_sem = refs[blocks:]
    x_copies = stack_copies(rows, x_all, x_sem, 0)
    begin(x_copies)
    finish(x_copies)
    for start, width in column_tiles(out.shape[1]):
        lanes = pl.ds(start, width)
        gate_vals = dot(x_all[...], gate[:, lanes])
        lift_vals = dot(x_all[...], lift[:, lanes])
        out[:, lanes] = (jax.nn.silu(gate_vals) * lift_vals).astype(NARROW)


def hidden_call(rows, gate, lift):
    count, depth = rows[0].shape
    tokens, width = count * len(rows), gate.shape[1]
    return call(
        functools.partial(hidden_kernel, len(rows)),
        [shape((tokens, width), NARROW)],
        [pltpu.VMEM((tokens, depth), NARROW), pltpu.SemaphoreType.DMA],
        4 * tokens * width * depth,
        *rows,
        gate,
        lift,
        specs=[ANY] * len(rows) + [VMEM] * 2,
    )[0]


def project(left, parts, outs):
    count = outs[0].shape[0]
    start = 0
    for part in parts:
        for offset, width in column_tiles(part.shape[1]):
            value = dot(left, part[:, pl.ds(offset, width)]).astype(NARROW)
            for j, out in enumerate(outs):
                out[:, pl.ds(start + offset, width)] = value[j * count : (j + 1) * count]
        start += part.shape[1]


def down_kernel(pieces, hidden, *refs):
    project(hidden[...], refs[:pieces], refs[pieces:])


def down_call(hidden, parts, count):
    tokens = hidden.shape[0]
    depth = sum(part.shape[1] for part in parts)
    members = tokens // count
    return call(
        functools.partial(down_kernel, len(parts)),
        [shape((count, depth), NARROW)] * members,
        [],
        2 * tokens * hidden.shape[1] * depth,
        hidden,
        *parts,
        specs=[VMEM] * (1 + len(parts)),
    )


def mix_in_kernel(blocks, with_stats, *refs):
    rows, weight, rest = refs[:blocks], refs[blocks], refs[blocks + 1 :]
    x_all, x_sem = rest[-2:]
    x_copies = stack_copies(rows, x_all, x_sem, 0)
    begin(x_copies)
    finish(x_copies)
    lifted = jax.nn.gelu(dot(x_all[...], weight[...]))
    rest[0][...] = lifted
    if with_stats:
        lane = lax.broadcasted_iota(jnp.int32, (lifted.shape[0], LANES), 1)
        sums = jnp.sum(lifted, axis=1, keepdims=True)
        squares = jnp.sum(lifted * lifted, axis=1, keepdims=True)
        both = jnp.where(lane == 0, sums, jnp.where(lane == 1, squares, 0.0))
        rest[1][...] = both.T[:SUBLANES]


def mix_in_call(rows, weight, with_stats):
    count, depth = rows[0].shape
    tokens, width = count * len(rows), weight.shape[1]
    outs = [shape((tokens, width), WIDE)]
    if with_stats:
        outs.append(shape((SUBLANES, tokens), WIDE))
    return call(
        functools.partial(mix_in_kernel, len(rows), with_stats),
        outs,
        [pltpu.VMEM((tokens, depth), NARROW), pltpu.SemaphoreType.DMA],
        2 * tokens * width * depth,
        *rows,
        weight,
        specs=[ANY] * len(rows) + [VMEM],
    )


def gated_kernel(members, channels, lifted, u_act, gain, shift, spatial, bias, *refs):
    stats = refs[:members]
    gated, normed = refs[members:]
    tokens = lifted.shape[0]
    count = tokens // members
    chips = members // CORES
    columns = []
    for mine in range(members):
        chip, core = mine // CORES, mine % CORES
        total = None
        for theirs in range(members):
            there = ((chip - theirs // CORES) % chips) * CORES + (core ^ (theirs % CORES))
            term = stats[theirs][:, there * count : (there + 1) * count]
            total = term if total is None else total + term
        columns.append(total)
    both = jnp.concatenate(columns, axis=1)
    both = jnp.concatenate([both] * (LANES // SUBLANES), axis=0).T
    centre = both[:, :1] / channels
    spread = both[:, 1:2] / channels - centre * centre
    scale = lax.rsqrt(spread + layer_epsilon)
    normed[...] = (
        (lifted[...] - centre) * scale * gain[...] + shift[...]
    ).astype(NARROW)
    rows = lax.broadcasted_iota(jnp.int32, (SPAN, SPAN), 0)
    cols = lax.broadcasted_iota(jnp.int32, (SPAN, SPAN), 1)
    for g in range(spatial.shape[0]):
        lanes = pl.ds(g * GROUP_DIM, GROUP_DIM)
        kept = jnp.where(rows >= cols, spatial[g].astype(WIDE), 0.0).astype(NARROW)
        stack = [normed[pl.ds(b * SPAN, SPAN), lanes] for b in range(tokens // SPAN)]
        mixed = dot(kept, jnp.concatenate(stack, axis=1)) + bias[:, g : g + 1]
        for b in range(tokens // SPAN):
            place = pl.ds(b * SPAN, SPAN)
            value = mixed[:, b * GROUP_DIM : (b + 1) * GROUP_DIM]
            gated[place, lanes] = (u_act[place, lanes] * value).astype(NARROW)


def gated_call(lifted, u_act, gain, shift, spatial, bias, stats, channels):
    tokens, width = lifted.shape
    members = len(stats)
    return call(
        functools.partial(gated_kernel, members, channels),
        [shape((tokens, width), NARROW)],
        [pltpu.VMEM((tokens, width), NARROW)],
        2 * tokens * width * SPAN,
        lifted,
        u_act,
        gain,
        shift,
        spatial,
        bias,
        *stats,
        specs=[VMEM] * (6 + members),
    )[0]


def own_kernel(order, stream, gain, gain_two, gain_three, rows, normed, two, three):
    width = stream.shape[1] // order.shape[0]
    for i in range(order.shape[0]):
        source, place = pl.ds(order[i] * width, width), pl.ds(i * width, width)
        rows[:, place] = stream[:, source]
        two[:, place] = gain_two[:, source]
        three[:, place] = gain_three[:, source]
    wide = rows[...].astype(WIDE)
    factor = lax.rsqrt(jnp.mean(wide * wide, axis=1, keepdims=True) + norm_epsilon)
    for i in range(order.shape[0]):
        source, place = pl.ds(order[i] * width, width), pl.ds(i * width, width)
        part = rows[:, place].astype(WIDE) * factor * gain[:, source]
        normed[:, place] = part.astype(NARROW)


def own_call(order, stream, gain, gain_two, gain_three):
    return call(
        own_kernel,
        [shape(stream.shape, NARROW)] * 2 + [shape(gain.shape, WIDE)] * 2,
        [],
        stream.size * 8,
        order,
        stream,
        gain,
        gain_two,
        gain_three,
        specs=[SMEM] + [VMEM] * 4,
    )


def norm_rows(row_block, scale_gain):
    widened = row_block.astype(WIDE)
    factor = lax.rsqrt(jnp.mean(widened * widened, axis=1, keepdims=True) + norm_epsilon)
    return (widened * factor * scale_gain).astype(NARROW)


def add_rows(rows, groups, scale):
    totals = []
    for terms in groups:
        total = terms[0].astype(WIDE)
        for term in terms[1:]:
            total = total + term.astype(WIDE)
        totals.append(total)
    total = jnp.concatenate(totals, axis=1) if len(totals) > 1 else totals[0]
    return (rows.astype(WIDE) + scale * total).astype(NARROW)


def make_body(sizes):
    def body(
        stream,
        gain_before,
        gain_after,
        proj_gate,
        proj_lift,
        proj_down,
        mixer_gain,
        mixer_u,
        mixer_v,
        layer_gain,
        layer_shift,
        spatial,
        spatial_shift,
        mixer_down,
    ):
        place = Layout(sizes)
        count, depth = stream.shape
        members = place.members
        row = lambda value: value.reshape(1, -1)
        gate = place.gather_weight(proj_gate, 0)
        lift = place.gather_weight(proj_lift, 0)
        down = place.gather_weight(proj_down, 1)
        v_mat = place.gather_weight(mixer_v, 0)
        u_mat = place.gather_weight(mixer_u, 0)
        m_down = place.gather_weight(mixer_down, 1, direct=True)
        late = place.parts(depth)

        def project_early(hidden, parts):
            groups = []
            for chosen in (parts[:-late], parts[-late:]):
                blocks = down_call(hidden, chosen, count)
                far = place.scatter_far(blocks)
                groups.append(place.scatter_near(blocks) + far)
            return groups

        rows, normed, mixer_gain, gain_after = own_call(
            place.order(depth), stream, row(gain_before), row(mixer_gain),
            row(gain_after),
        )
        normed = place.gather_rows(normed)
        gate = pack_call(gate, 0)
        lift = pack_call(lift, 0)
        hidden = hidden_call(normed, gate, lift)
        groups = project_early(hidden, down)
        first = add_rows(rows, groups, 0.5)

        normed = place.gather_rows(norm_rows(first, mixer_gain))
        lifted, stats = mix_in_call(normed, pack_call(v_mat, 0), True)
        stats = place.share_stats(stats)
        (u_act,) = mix_in_call(normed, pack_call(u_mat, 0), False)
        gated = gated_call(
            lifted, u_act, row(layer_gain), row(layer_shift), spatial,
            spatial_shift.T, stats, layer_gain.shape[0] * members,
        )
        groups = project_early(gated, m_down)
        second = add_rows(first, groups, 1.0)

        normed = norm_rows(second, gain_after)
        half = count // HALVES
        cuts = [normed[i * half : (i + 1) * half] for i in range(HALVES)]
        far = [place.pass_rows(cut) for cut in cuts]
        near = [normed, place.shift_tp(normed, 0, 1)]
        down = pack_call(down, 1)
        hidden = hidden_call(near, gate, lift)
        blocks = down_call(hidden, [down], count)
        terms = [term.astype(WIDE) for term in place.scatter_near(blocks)]
        total = terms[0] + terms[1]
        sums = []
        for i in range(HALVES):
            hidden = hidden_call(far[i], gate, lift)
            blocks = down_call(hidden, [down], half)
            terms = place.scatter_far([None] * CORES + list(blocks))
            sums.append(sum(term.astype(WIDE) for term in terms))
        total = total + jnp.concatenate(sums, axis=0)
        return place.from_own((second.astype(WIDE) + 0.5 * total).astype(NARROW))

    return body


def solution(mesh):
    sizes = dict(mesh.shape)
    placed = (
        P(("rep", "fs", "tp"), None),
        P(),
        P(),
        P("fs", "tp"),
        P("fs", "tp"),
        P("tp", "fs"),
        P(),
        P("fs", "tp"),
        P("fs", "tp"),
        P("tp"),
        P("tp"),
        P("tp", None, None),
        P("tp", None),
        P("tp", "fs"),
    )
    return jax.shard_map(
        make_body(sizes),
        mesh=mesh,
        in_specs=placed,
        out_specs=P(("rep", "fs", "tp"), None),
        check_vma=False,
    )
```

```python
import functools

import jax
import jax.numpy as jnp
from jax import lax
from jax.experimental import pallas as pl
from jax.experimental.pallas import tpu as pltpu
from jax.sharding import PartitionSpec as P


GROUP_DIM = 128
SPAN = 128
CORES = 2
LANES = 128
SUBLANES = 8
TILE = 256
HALVES = 2

norm_epsilon = 1e-06
layer_epsilon = 1e-05


ANY = pl.BlockSpec(memory_space=pl.ANY)
VMEM = pl.BlockSpec(memory_space=pltpu.VMEM)
SMEM = pl.BlockSpec(memory_space=pltpu.SMEM)
WIDE = jnp.float32
NARROW = jnp.bfloat16


def rotation(count, shift):
    return [(i, (i + shift) % count) for i in range(count)]


class Layout:
    def __init__(self, sizes):
        self.reps = sizes["rep"]
        self.shards = sizes["fs"]
        self.chips = sizes["tp"] // CORES
        self.members = sizes["tp"]
        self.rep = lax.axis_index("rep")
        self.fs = lax.axis_index("fs")

    def shift_fs(self, value, shift):
        return lax.ppermute(value, "fs", rotation(self.shards, shift))

    def shift_rep(self, value, shift):
        return lax.ppermute(value, "rep", rotation(self.reps, shift))

    def shift_tp(self, value, chip_shift, core_flip):
        pairs = [
            (
                chip * CORES + core,
                ((chip + chip_shift) % self.chips) * CORES + (core ^ core_flip),
            )
            for chip in range(self.chips)
            for core in range(CORES)
        ]
        return lax.ppermute(value, "tp", pairs)

    def parts(self, depth):
        return 1 if depth % (self.shards * self.reps * LANES) else self.reps

    def blocks(self, depth):
        reps = self.parts(depth)
        order = [self.fs * reps + j for j in range(reps)]
        for slot in range(1, self.shards):
            owner = (self.fs - slot + self.shards) % self.shards
            for j in range(reps):
                piece = (self.rep - j + self.reps) % self.reps if reps > 1 else 0
                order.append(owner * reps + piece)
        return order

    def order(self, depth):
        reps = self.parts(depth)
        slot = jnp.arange(self.shards, dtype=jnp.int32)[:, None]
        j = jnp.arange(reps, dtype=jnp.int32)[None]
        owner = (self.fs - slot + self.shards) % self.shards
        turned = (self.rep - j + self.reps) % self.reps if reps > 1 else j
        piece = jnp.where(slot == 0, j, turned)
        return (owner * reps + piece).reshape(-1).astype(jnp.int32)

    def from_own(self, value):
        order = self.blocks(value.shape[-1])
        width = value.shape[-1] // len(order)
        out = jnp.zeros_like(value)
        for i, index in enumerate(order):
            part = value[:, i * width : (i + 1) * width]
            out = lax.dynamic_update_slice_in_dim(out, part, index * width, axis=1)
        return out

    def gather_weight(self, shard, axis, direct=False):
        reps = self.parts(shard.shape[axis] * self.shards)
        width = shard.shape[axis] // reps
        first = self.rep * width if reps > 1 else 0
        piece = lax.dynamic_slice_in_dim(shard, first, width, axis=axis)
        moving, out = piece, [shard]
        for slot in range(1, self.shards):
            if direct and slot == self.shards - 1:
                out.append(self.shift_fs(shard, -1))
                break
            moving = self.shift_fs(moving, 1)
            out.append(moving)
            for j in range(1, reps):
                out.append(self.shift_rep(moving, j))
        return out

    def gather_rows(self, rows):
        near = self.shift_tp(rows, 0, 1)
        out = [rows, near]
        for j in range(1, self.chips):
            far = self.shift_tp(rows, j, 0)
            out.extend([far, self.shift_tp(far, 0, 1)])
        return out

    def pass_rows(self, rows):
        out = []
        for j in range(1, self.chips):
            far = self.shift_tp(rows, j, 0)
            out.extend([far, self.shift_tp(far, 0, 1)])
        return out

    def scatter_far(self, blocks):
        terms = []
        for j in range(self.chips - 1, 0, -1):
            near = self.shift_tp(blocks[CORES * j + 1], 0, 1)
            pair = (blocks[CORES * j].astype(WIDE) + near.astype(WIDE)).astype(NARROW)
            terms.append(self.shift_tp(pair, -j, 0))
        return terms

    def scatter_near(self, blocks):
        return [blocks[0], self.shift_tp(blocks[1], 0, 1)]

    def share_stats(self, stats):
        out = []
        for j in range(self.chips):
            for flip in range(CORES):
                same = j == 0 and flip == 0
                out.append(stats if same else self.shift_tp(stats, j, flip))
        return out


def dot(left, right):
    return jnp.dot(left, right, preferred_element_type=WIDE)


def column_tiles(width):
    if width % LANES or width <= TILE:
        return [(0, width)]
    starts = list(range(0, width - TILE + 1, TILE))
    ends = starts[1:] + [width]
    return [(a, b - a) for a, b in zip(starts, ends)]


def call(kernel, outs, scratch, flops, *args, specs, out_specs=None, room=24):
    return pl.pallas_call(
        kernel,
        out_shape=outs,
        in_specs=specs,
        out_specs=out_specs or [VMEM] * len(outs),
        scratch_shapes=scratch,
        compiler_params=pltpu.CompilerParams(vmem_limit_bytes=room * 2**20),
        cost_estimate=pl.CostEstimate(flops=flops, transcendentals=0, bytes_accessed=0),
    )(*args)


def shape(dims, kind):
    return jax.ShapeDtypeStruct(dims, kind)


def stack_copies(refs, target, sem, axis):
    out, start = [], 0
    for ref in refs:
        place = pl.ds(start, ref.shape[axis])
        start += ref.shape[axis]
        at = (place, slice(None)) if axis == 0 else (slice(None), place)
        out.append(pltpu.make_async_copy(ref, target.at[at], sem))
    return out


def begin(copies):
    for copy in copies:
        copy.start()


def finish(copies):
    for copy in copies:
        copy.wait()


def pack_kernel(axis, *refs):
    copies = stack_copies(refs[:-2], refs[-2], refs[-1], axis)
    begin(copies)
    finish(copies)


def pack_call(parts, axis):
    dims = list(parts[0].shape)
    dims[axis] = sum(part.shape[axis] for part in parts)
    return call(
        functools.partial(pack_kernel, axis),
        [shape(tuple(dims), NARROW)],
        [pltpu.SemaphoreType.DMA],
        1000000,
        *parts,
        specs=[ANY] * len(parts),
        out_specs=[ANY],
    )[0]


def hidden_kernel(blocks, *refs):
    rows = refs[:blocks]
    gate, lift, out, x_all, x_sem = refs[blocks:]
    x_copies = stack_copies(rows, x_all, x_sem, 0)
    begin(x_copies)
    finish(x_copies)
    for start, width in column_tiles(out.shape[1]):
        lanes = pl.ds(start, width)
        gate_vals = dot(x_all[...], gate[:, lanes])
        lift_vals = dot(x_all[...], lift[:, lanes])
        out[:, lanes] = (jax.nn.silu(gate_vals) * lift_vals).astype(NARROW)


def hidden_call(rows, gate, lift):
    count, depth = rows[0].shape
    tokens, width = count * len(rows), gate.shape[1]
    return call(
        functools.partial(hidden_kernel, len(rows)),
        [shape((tokens, width), NARROW)],
        [pltpu.VMEM((tokens, depth), NARROW), pltpu.SemaphoreType.DMA],
        4 * tokens * width * depth,
        *rows,
        gate,
        lift,
        specs=[ANY] * len(rows) + [VMEM] * 2,
    )[0]


def project(left, parts, outs):
    count = outs[0].shape[0]
    start = 0
    for part in parts:
        for offset, width in column_tiles(part.shape[1]):
            value = dot(left, part[:, pl.ds(offset, width)]).astype(NARROW)
            for j, out in enumerate(outs):
                out[:, pl.ds(start + offset, width)] = value[j * count : (j + 1) * count]
        start += part.shape[1]


def down_kernel(pieces, hidden, *refs):
    project(hidden[...], refs[:pieces], refs[pieces:])


def whole_kernel(turn, hidden, part, *outs):
    width = part.shape[1] // turn.shape[0]
    count = outs[0].shape[0]
    for i in range(turn.shape[0]):
        piece = part[:, pl.ds(turn[i] * width, width)]
        value = dot(hidden[...], piece).astype(NARROW)
        for j, out in enumerate(outs):
            out[:, pl.ds(i * width, width)] = value[j * count : (j + 1) * count]


def whole_call(hidden, part, count, turn):
    tokens, depth = hidden.shape[0], part.shape[1]
    return call(
        whole_kernel,
        [shape((count, depth), NARROW)] * (tokens // count),
        [],
        2 * tokens * hidden.shape[1] * depth,
        turn,
        hidden,
        part,
        specs=[SMEM] + [VMEM] * 2,
    )


def down_call(hidden, parts, count):
    tokens = hidden.shape[0]
    depth = sum(part.shape[1] for part in parts)
    members = tokens // count
    return call(
        functools.partial(down_kernel, len(parts)),
        [shape((count, depth), NARROW)] * members,
        [],
        2 * tokens * hidden.shape[1] * depth,
        hidden,
        *parts,
        specs=[VMEM] * (1 + len(parts)),
    )


def activate(x_all, weight, out, stats):
    lifted = jax.nn.gelu(dot(x_all[...], weight[...]))
    out[...] = lifted
    if stats is not None:
        lane = lax.broadcasted_iota(jnp.int32, (lifted.shape[0], LANES), 1)
        sums = jnp.sum(lifted, axis=1, keepdims=True)
        squares = jnp.sum(lifted * lifted, axis=1, keepdims=True)
        both = jnp.where(lane == 0, sums, jnp.where(lane == 1, squares, 0.0))
        stats[...] = both.T[:SUBLANES]


def v_kernel(blocks, *refs):
    rows, (weight, out, stats, x_all, x_sem) = refs[:blocks], refs[blocks:]
    x_copies = stack_copies(rows, x_all, x_sem, 0)
    begin(x_copies)
    finish(x_copies)
    activate(x_all, weight, out, stats)


def v_call(rows, weight):
    count, depth = rows[0].shape
    tokens, width = count * len(rows), weight.shape[1]
    return call(
        functools.partial(v_kernel, len(rows)),
        [
            shape((tokens, width), WIDE),
            shape((SUBLANES, tokens), WIDE),
            shape((tokens, depth), NARROW),
        ],
        [pltpu.SemaphoreType.DMA],
        2 * tokens * width * depth,
        *rows,
        weight,
        specs=[ANY] * len(rows) + [VMEM],
    )


def u_kernel(x_all, weight, out):
    activate(x_all, weight, out, None)


def u_call(x_all, weight):
    tokens, depth = x_all.shape
    width = weight.shape[1]
    return call(
        u_kernel,
        [shape((tokens, width), WIDE)],
        [],
        2 * tokens * width * depth,
        x_all,
        weight,
        specs=[VMEM] * 2,
    )[0]


def gated_kernel(members, channels, lifted, u_act, gain, shift, spatial, bias, *refs):
    stats = refs[:members]
    gated, normed = refs[members:]
    tokens = lifted.shape[0]
    count = tokens // members
    chips = members // CORES
    columns = []
    for mine in range(members):
        chip, core = mine // CORES, mine % CORES
        total = None
        for theirs in range(members):
            there = ((chip - theirs // CORES) % chips) * CORES + (core ^ (theirs % CORES))
            term = stats[theirs][:, there * count : (there + 1) * count]
            total = term if total is None else total + term
        columns.append(total)
    both = jnp.concatenate(columns, axis=1)
    both = jnp.concatenate([both] * (LANES // SUBLANES), axis=0).T
    centre = both[:, :1] / channels
    spread = both[:, 1:2] / channels - centre * centre
    scale = lax.rsqrt(spread + layer_epsilon)
    normed[...] = (
        (lifted[...] - centre) * scale * gain[...] + shift[...]
    ).astype(NARROW)
    rows = lax.broadcasted_iota(jnp.int32, (SPAN, SPAN), 0)
    cols = lax.broadcasted_iota(jnp.int32, (SPAN, SPAN), 1)
    for g in range(spatial.shape[0]):
        lanes = pl.ds(g * GROUP_DIM, GROUP_DIM)
        kept = jnp.where(rows >= cols, spatial[g].astype(WIDE), 0.0).astype(NARROW)
        stack = [normed[pl.ds(b * SPAN, SPAN), lanes] for b in range(tokens // SPAN)]
        mixed = dot(kept, jnp.concatenate(stack, axis=1)) + bias[:, g : g + 1]
        for b in range(tokens // SPAN):
            place = pl.ds(b * SPAN, SPAN)
            value = mixed[:, b * GROUP_DIM : (b + 1) * GROUP_DIM]
            gated[place, lanes] = (u_act[place, lanes] * value).astype(NARROW)


def gated_call(lifted, u_act, gain, shift, spatial, bias, stats, channels):
    tokens, width = lifted.shape
    members = len(stats)
    return call(
        functools.partial(gated_kernel, members, channels),
        [shape((tokens, width), NARROW)],
        [pltpu.VMEM((tokens, width), NARROW)],
        2 * tokens * width * SPAN,
        lifted,
        u_act,
        gain,
        shift,
        spatial,
        bias,
        *stats,
        specs=[VMEM] * (6 + members),
    )[0]


def own_kernel(order, stream, gain, gain_two, gain_three, rows, normed, two, three):
    width = stream.shape[1] // order.shape[0]
    for i in range(order.shape[0]):
        source, place = pl.ds(order[i] * width, width), pl.ds(i * width, width)
        rows[:, place] = stream[:, source]
        two[:, place] = gain_two[:, source]
        three[:, place] = gain_three[:, source]
    wide = rows[...].astype(WIDE)
    factor = lax.rsqrt(jnp.mean(wide * wide, axis=1, keepdims=True) + norm_epsilon)
    for i in range(order.shape[0]):
        source, place = pl.ds(order[i] * width, width), pl.ds(i * width, width)
        part = rows[:, place].astype(WIDE) * factor * gain[:, source]
        normed[:, place] = part.astype(NARROW)


def own_call(order, stream, gain, gain_two, gain_three):
    return call(
        own_kernel,
        [shape(stream.shape, NARROW)] * 2 + [shape(gain.shape, WIDE)] * 2,
        [],
        stream.size * 8,
        order,
        stream,
        gain,
        gain_two,
        gain_three,
        specs=[SMEM] + [VMEM] * 4,
    )


def norm_rows(row_block, scale_gain):
    widened = row_block.astype(WIDE)
    factor = lax.rsqrt(jnp.mean(widened * widened, axis=1, keepdims=True) + norm_epsilon)
    return (widened * factor * scale_gain).astype(NARROW)


def add_rows(rows, groups, scale):
    totals = []
    for terms in groups:
        total = terms[0].astype(WIDE)
        for term in terms[1:]:
            total = total + term.astype(WIDE)
        totals.append(total)
    total = jnp.concatenate(totals, axis=1) if len(totals) > 1 else totals[0]
    return (rows.astype(WIDE) + scale * total).astype(NARROW)


def make_body(sizes):
    def body(
        stream,
        gain_before,
        gain_after,
        proj_gate,
        proj_lift,
        proj_down,
        mixer_gain,
        mixer_u,
        mixer_v,
        layer_gain,
        layer_shift,
        spatial,
        spatial_shift,
        mixer_down,
    ):
        place = Layout(sizes)
        count, depth = stream.shape
        members = place.members
        row = lambda value: value.reshape(1, -1)
        gate = place.gather_weight(proj_gate, 0)
        lift = place.gather_weight(proj_lift, 0)
        down = place.gather_weight(proj_down, 1)
        v_mat = place.gather_weight(mixer_v, 0)
        u_mat = place.gather_weight(mixer_u, 0)
        m_down = place.gather_weight(mixer_down, 1, direct=True)
        late = place.parts(depth)

        order = place.order(depth)
        turn = order[-late:] % late

        def project_early(stage, hidden, parts):
            groups = []
            for group, chosen in parts:
                if stage == 2 and group == "f":
                    blocks = whole_call(hidden, chosen[0], count, turn)
                else:
                    blocks = down_call(hidden, chosen, count)
                far = place.scatter_far(blocks)
                groups.append(place.scatter_near(blocks) + far)
            return groups

        rows, normed, mixer_gain, gain_after = own_call(
            order, stream, row(gain_before), row(mixer_gain),
            row(gain_after),
        )
        normed = place.gather_rows(normed)
        gate = pack_call(gate, 0)
        lift = pack_call(lift, 0)
        hidden = hidden_call(normed, gate, lift)
        groups = project_early(1, hidden, (("e", down[:-late]), ("f", down[-late:])))
        first = add_rows(rows, groups, 0.5)

        normed = place.gather_rows(norm_rows(first, mixer_gain))
        lifted, stats, joined = v_call(normed, pack_call(v_mat, 0))
        stats = place.share_stats(stats)
        u_act = u_call(joined, pack_call(u_mat, 0))
        gated = gated_call(
            lifted, u_act, row(layer_gain), row(layer_shift), spatial,
            spatial_shift.T, stats, layer_gain.shape[0] * members,
        )
        groups = project_early(
            2, gated,
            (
                ("e", m_down[: -late - 1]),
                ("g", m_down[-late - 1 : -1]),
                ("f", m_down[-1:]),
            ),
        )
        second = add_rows(first, groups, 1.0)

        normed = norm_rows(second, gain_after)
        half = count // HALVES
        cuts = [normed[i * half : (i + 1) * half] for i in range(HALVES)]
        far = [place.pass_rows(cut) for cut in cuts]
        near = [normed, place.shift_tp(normed, 0, 1)]
        down = pack_call(down, 1)
        hidden = hidden_call(near, gate, lift)
        blocks = down_call(hidden, [down], count)
        terms = [term.astype(WIDE) for term in place.scatter_near(blocks)]
        base = second.astype(WIDE) + 0.5 * (terms[0] + terms[1])
        results = []
        for i in range(HALVES):
            hidden = hidden_call(far[i], gate, lift)
            blocks = down_call(hidden, [down], half)
            terms = place.scatter_far([None] * CORES + list(blocks))
            total = sum(term.astype(WIDE) for term in terms)
            rows = base[i * half : (i + 1) * half] + 0.5 * total
            results.append(place.from_own(rows.astype(NARROW)))
        return jnp.concatenate(results, axis=0)

    return body


def solution(mesh):
    sizes = dict(mesh.shape)
    placed = (
        P(("rep", "fs", "tp"), None),
        P(),
        P(),
        P("fs", "tp"),
        P("fs", "tp"),
        P("tp", "fs"),
        P(),
        P("fs", "tp"),
        P("fs", "tp"),
        P("tp"),
        P("tp"),
        P("tp", None, None),
        P("tp", None),
        P("tp", "fs"),
    )
    return jax.shard_map(
        make_body(sizes),
        mesh=mesh,
        in_specs=placed,
        out_specs=P(("rep", "fs", "tp"), None),
        check_vma=False,
    )
```
